32 devices in a mesh: ep: 4 (over y, x), tp: 8 (over z, core).
Axes of the slice: x: 2, y: 2, z: 4, core: 2. Of those that a mesh axis runs over, the one named last changes fastest.
Arguments:
- query_rows: bfloat16 [4096, 2048], P('ep', 'tp'), may hold values from -6 to 6
- key_rows: bfloat16 [4096, 2048], P('ep', 'tp'), may hold values from -6 to 6
- value_rows: bfloat16 [4096, 4096], P('ep', 'tp'), may hold values from -6 to 6
- gate_rows: bfloat16 [4096, 4096], P('ep', 'tp'), may hold values from -6 to 6
- log_decay: float32 [16, 4096], P('tp', 'ep'), may hold values from -1.5 to 0
- out_weight: bfloat16 [4096, 2048], P('tp'), may hold values from -0.09375 to 0.09375
- channel_input: bfloat16 [1536, 2048], P(('ep', 'tp')), may hold values from -6 to 6
- norm_gain: float32 [2048], replicated, may hold values from 0.1 to 1.9
- routes: int32 [1536, 2], P(('ep', 'tp')), may hold values from 0 to 7, all different within a row; in each aligned block of 48 rows (0 to 47, 48 to 95, ...) at most 16 rows name the same one
- route_weight: float32 [1536, 2], P(('ep', 'tp')), may hold values from 0.2 to 1.5
- expert_gate: bfloat16 [8, 2048, 2048], P('ep', None, 'tp'), may hold values from -0.125 to 0.125
- expert_up: bfloat16 [8, 2048, 2048], P('ep', None, 'tp'), may hold values from -0.125 to 0.125
- expert_down: bfloat16 [8, 2048, 2048], P('ep', 'tp'), may hold values from -0.125 to 0.125
- shared_gate: bfloat16 [2048, 2048], P(None, 'tp'), may hold values from -0.125 to 0.125
- shared_up: bfloat16 [2048, 2048], P(None, 'tp'), may hold values from -0.125 to 0.125
- shared_down: bfloat16 [2048, 2048], P('tp'), may hold values from -0.125 to 0.125
Outputs:
- mixer_out: bfloat16 [4096, 2048], P(('ep', 'tp'))
- channel_out: bfloat16 [1536, 2048], P(('ep', 'tp'))
The draws below stay inside these ranges and needn't reach their ends.
Inputs may be any that keep to these rules, and one draw needn't show every extreme that they name: `routes`: each row names 2 different experts; among the rows of one device no expert is named more than 16 times, a bound that some block reaches.
All inputs are finite; a program needn't handle non-finite values.
Results may differ from the reference program's by a relative error of at most 0.02.
Values may be sent and summed in bfloat16 or wider, within the bound.
A program may use at most 128 MiB of HBM per device.

```python
import math
import jax
import jax.numpy as jnp
import numpy as np
from jax import lax

D = 2048
RETENTION_HEADS = 16
DK = 128
DV = 256
BLOCK = 128
TOK_A = 1024
FF = 2048
TOPK = 2
T_M = 48
SEQUENCE_LENGTH = 4096
QK_WIDTH = 2048
V_WIDTH = 4096
EXPERTS = 8
TOKENS_M = 1536
CAP = 16
N_EP = 4
N_TP = 8


def draw_log_decay(key, part):
    key_pieces_list = jax.random.split(jax.random.fold_in(key, 11), 7)
    slow_share = 0.5
    slow_heads = jax.random.uniform(key_pieces_list[0], (RETENTION_HEADS,)) < slow_share
    whole_loss = jax.random.uniform(key_pieces_list[1], (RETENTION_HEADS,), minval=0.1, maxval=0.5)
    fast_rate = jax.random.uniform(key_pieces_list[2], (RETENTION_HEADS,), minval=1.0 / 100.0, maxval=1.0 / 30.0)
    decay_rate = jnp.where(slow_heads, whole_loss / SEQUENCE_LENGTH, fast_rate)
    span_count = SEQUENCE_LENGTH // TOK_A
    block_factor = jnp.exp(jax.random.uniform(key_pieces_list[3], (RETENTION_HEADS, span_count), minval=-0.7, maxval=0.7))
    block_factor = jnp.repeat(block_factor, TOK_A, axis=1)
    jitter = jax.random.uniform(key_pieces_list[4], (RETENTION_HEADS, SEQUENCE_LENGTH), minval=0.5, maxval=1.5)
    steady_level = -(decay_rate[:, None] * block_factor * jitter)
    surge_position = jax.random.randint(key_pieces_list[5], (RETENTION_HEADS, 2), 0, SEQUENCE_LENGTH)
    surge_extent = jnp.log(jax.random.uniform(key_pieces_list[6], (RETENTION_HEADS, 2), minval=0.5, maxval=0.8))
    head_number = jnp.broadcast_to(jnp.arange(RETENTION_HEADS)[:, None], (RETENTION_HEADS, 2))
    surge_list = jnp.zeros((RETENTION_HEADS, SEQUENCE_LENGTH), jnp.float32).at[head_number, surge_position].add(surge_extent)
    return (steady_level + surge_list).astype(jnp.float32)


def block_scale(own_key, shape, cuts, least, largest):
    loudness = 1.0
    for dim, shards_of in cuts:
        steps = jax.random.uniform(jax.random.fold_in(jax.random.fold_in(own_key, 6), dim), (shards_of,), jnp.float32, least / len(cuts), largest / len(cuts))
        loudness = loudness * jnp.repeat(jnp.exp(steps), shape[dim] // shards_of).reshape((-1,) + (1,) * (len(shape) - 1 - dim))
    return loudness


def shared_out(rng, own, number, rows, number_of, top, most, slope):
    sequence = jax.random.permutation(rng, number_of)
    crowded, usual = shares(number_of, rows * top, most, slope, True), shares(number_of, rows * top, most, slope, False)
    places = jnp.arange(number_of)

    def named(tallies, rotation):
        used = int((tallies > 0).sum())
        fixed = max(1, used // 4)
        passed = fixed + (places - fixed + rotation * (used - fixed)) % max(1, number_of - fixed)
        return jnp.zeros((number_of,), jnp.int32).at[sequence[jnp.where(places < fixed, places, passed)]].set(jnp.asarray(tallies, jnp.int32))

    tallies = jnp.where(number % 4 == 0, named(crowded, number // 4), named(usual, number - number // 4 - 1))
    mixed = jax.random.permutation(jax.random.fold_in(own, 3), number_of)
    giver, sink = mixed[0:number_of // 2 * 2:2], mixed[1:number_of // 2 * 2:2]
    slack = jnp.minimum(tallies[giver] - 1, most - tallies[sink]) // 2
    slack = jnp.where((giver == sequence[0]) | (sink == sequence[0]) | (tallies[sink] == 0), 0, jnp.maximum(slack, 0))
    passed = jax.random.randint(jax.random.fold_in(own, 4), (number_of // 2,), 0, 1 << 20) % (slack + 1)
    tallies = tallies.at[giver].add(-passed).at[sink].add(passed)
    members = jnp.searchsorted(jnp.cumsum(tallies), jnp.arange(rows * top), side="right").astype(jnp.int32)
    listing = members.reshape(top, rows).T
    listing = listing[jax.random.permutation(jax.random.fold_in(own, 1), rows)]
    rotation = jax.random.randint(jax.random.fold_in(own, 2), (rows, 1), 0, top)
    return jnp.take_along_axis(listing, (jnp.arange(top)[None, :] + rotation) % top, axis=1)


def shares(amount, total, most, slope, full):
    loads = [(1 << 20) // math.isqrt(standing ** slope) + 1 for standing in range(1, amount + 1)]
    largest = most if full else min(most, max(-(-total // amount), total * loads[0] // sum(loads)))
    least = 1 if total - largest >= amount - 1 else 0
    given, spare = [largest] + [least] * (amount - 1), total - largest - least * (amount - 1)
    while spare > 0:
        free = [i for i in range(1, amount) if given[i] < largest] or [i for i in range(1, amount) if given[i] < most]
        whole, left = sum([loads[i] for i in free]), spare
        for i in free:
            addition = min(most - given[i], max(1, left * loads[i] // whole), spare)
            given[i] = given[i] + addition
            spare = spare - addition
    return np.array(given)


def noise(key, shape, scale, most, pieces=(), kind=jnp.bfloat16):
    values = scale * jax.random.normal(key, shape, jnp.float32)
    if pieces:
        values = values * block_scale(key, shape, pieces, -0.22, 0.18)
    return jnp.clip(values, -most, most).astype(kind)


def setup_inputs(seed: int = 0) -> dict:
    arg_keys = jax.random.split(jax.random.key(seed), 17)
    query_rows = noise(arg_keys[0], (SEQUENCE_LENGTH, QK_WIDTH), 1.0, 6.0, ((0, 4), (1, 8)))
    key_rows = noise(arg_keys[1], (SEQUENCE_LENGTH, QK_WIDTH), 1.0, 6.0, ((0, 4), (1, 8)))
    value_rows = noise(arg_keys[2], (SEQUENCE_LENGTH, V_WIDTH), 1.0, 6.0, ((0, 4), (1, 8)))
    gate_rows = noise(arg_keys[3], (SEQUENCE_LENGTH, V_WIDTH), 1.0, 6.0, ((0, 4), (1, 8)))
    log_decay = draw_log_decay(jax.random.fold_in(arg_keys[16], 71), 0)
    out_weight = noise(arg_keys[5], (V_WIDTH, D), V_WIDTH ** -0.5, 0.09375, ((0, 8),))
    channel_input = noise(arg_keys[6], (TOKENS_M, D), 1.0, 6.0, ((0, 32),))
    norm_gain = jnp.clip(1.0 + 0.18 * jax.random.normal(arg_keys[7], (D,), jnp.float32), 0.1, 1.9)
    routes_keys = jax.random.split(jax.random.fold_in(arg_keys[8], 1), TOKENS_M // T_M)
    routes_turns = jax.random.permutation(jax.random.fold_in(arg_keys[8], 3), TOKENS_M // T_M)
    routes = jax.vmap(lambda own, number: shared_out(jax.random.fold_in(arg_keys[8], 2), own, number, T_M, EXPERTS, TOPK, CAP, 1))(routes_keys, routes_turns).reshape((TOKENS_M, TOPK))
    route_weight = jnp.clip(0.2 + 1.3 * jax.random.uniform(arg_keys[9], (TOKENS_M, TOPK), jnp.float32) ** block_scale(arg_keys[9], (TOKENS_M, TOPK), ((0, 32),), -0.2, 0.2), 0.2, 1.5)
    expert_gate = noise(arg_keys[10], (EXPERTS, D, FF), D ** -0.5, 0.125, ((0, 4), (2, 8)))
    expert_up = noise(arg_keys[11], (EXPERTS, D, FF), D ** -0.5, 0.125, ((0, 4), (2, 8)))
    expert_down = noise(arg_keys[12], (EXPERTS, FF, D), FF ** -0.5, 0.125, ((0, 4), (1, 8)))
    shared_gate = noise(arg_keys[13], (D, FF), D ** -0.5, 0.125, ((1, 8),))
    shared_up = noise(arg_keys[14], (D, FF), D ** -0.5, 0.125, ((1, 8),))
    shared_down = noise(arg_keys[15], (FF, D), FF ** -0.5, 0.125, ((0, 8),))
    return {"query_rows": query_rows, "key_rows": key_rows, "value_rows": value_rows, "gate_rows": gate_rows, "log_decay": log_decay, "out_weight": out_weight, "channel_input": channel_input, "norm_gain": norm_gain, "routes": routes, "route_weight": route_weight, "expert_gate": expert_gate, "expert_up": expert_up, "expert_down": expert_down, "shared_gate": shared_gate, "shared_up": shared_up, "shared_down": shared_down}


epsilon = 1e-06
turn_base = 10000.0

def turn_heads(rows, position):
    half_width = rows.shape[-1] // 2
    inverse = turn_base ** (-jnp.arange(half_width, dtype=jnp.float32) / half_width)
    angles = position[:, None] * inverse[None, :]
    cosine = jnp.cos(angles)[:, None, :]
    sine = jnp.sin(angles)[:, None, :]
    widened = rows.astype(jnp.float32)
    first_half = widened[..., :half_width]
    second_half = widened[..., half_width:]
    turned = jnp.concatenate([first_half * cosine - second_half * sine, second_half * cosine + first_half * sine], axis=-1)
    return turned.astype(jnp.bfloat16)

def blocked_product(left, right, parts):
    width = right.shape[0] // parts

    def add_block(index, total):
        columns = lax.dynamic_slice_in_dim(left, index * width, width, 1)
        block_rows = lax.dynamic_slice_in_dim(right, index * width, width, 0)
        partial_sum = jnp.dot(columns, block_rows, preferred_element_type=jnp.float32).astype(jnp.bfloat16)
        partial_sum = lax.optimization_barrier(partial_sum)
        return total + partial_sum.astype(jnp.float32)
    return lax.fori_loop(0, parts, add_block, jnp.zeros((left.shape[0], right.shape[1]), jnp.float32))

def swiglu_hidden(rows, gate_weight, up_weight):
    gate_part = jnp.dot(rows, gate_weight, preferred_element_type=jnp.float32)
    up_part = jnp.dot(rows, up_weight, preferred_element_type=jnp.float32)
    return (jax.nn.silu(gate_part) * up_part).astype(jnp.bfloat16)

def retention(queries, keys_turned, values, log_decay):
    block_count = SEQUENCE_LENGTH // BLOCK
    query_blocks = queries.reshape(block_count, BLOCK, RETENTION_HEADS, DK)
    key_blocks = keys_turned.reshape(block_count, BLOCK, RETENTION_HEADS, DK)
    value_blocks = values.reshape(block_count, BLOCK, RETENTION_HEADS, DV)
    decay_blocks = jnp.transpose(log_decay.reshape(RETENTION_HEADS, block_count, BLOCK), (1, 0, 2))
    lower = jnp.arange(BLOCK)[:, None] >= jnp.arange(BLOCK)[None, :]
    highest = lax.Precision.HIGHEST

    def advance(state, inputs):
        query_block, key_block, value_block, decay_block = inputs
        running = jnp.cumsum(decay_block, axis=1)
        query_wide = query_block.astype(jnp.float32)
        key_wide = key_block.astype(jnp.float32)
        value_wide = value_block.astype(jnp.float32)
        scores = jnp.einsum('ihk,jhk->hij', query_wide, key_wide, precision=highest)
        spread = running[:, :, None] - running[:, None, :]
        weights = jnp.where(lower, scores * jnp.exp(jnp.where(lower, spread, 0.0)), 0.0).astype(jnp.bfloat16)
        intra = jnp.einsum('hij,jhe->ihe', weights.astype(jnp.float32), value_wide, precision=highest)
        query_decayed = query_wide * jnp.exp(running).T[:, :, None]
        inter = jnp.einsum('ihk,hke->ihe', query_decayed, state, precision=highest)
        block_end = running[:, -1]
        key_decayed = key_wide * jnp.exp(block_end[:, None] - running).T[:, :, None]
        update = jnp.einsum('jhk,jhe->hke', key_decayed, value_wide, precision=highest)
        new_state = jnp.exp(block_end)[:, None, None] * state + update
        return (new_state, intra + inter)
    start_state = jnp.zeros((RETENTION_HEADS, DK, DV), jnp.float32)
    _, outputs = lax.scan(advance, start_state, (query_blocks, key_blocks, value_blocks, decay_blocks))
    return outputs.reshape(SEQUENCE_LENGTH, RETENTION_HEADS, DV)

def reference(query_rows, key_rows, value_rows, gate_rows, log_decay, out_weight, channel_input, norm_gain, routes, route_weight, expert_gate, expert_up, expert_down, shared_gate, shared_up, shared_down):
    position = jnp.arange(SEQUENCE_LENGTH, dtype=jnp.int32).astype(jnp.float32)
    queries = turn_heads(query_rows.reshape(SEQUENCE_LENGTH, RETENTION_HEADS, DK), position)
    keys_turned = turn_heads(key_rows.reshape(SEQUENCE_LENGTH, RETENTION_HEADS, DK), position)
    retained = retention(queries, keys_turned, value_rows.reshape(SEQUENCE_LENGTH, RETENTION_HEADS, DV), log_decay)
    scaled = retained * lax.rsqrt(lax.optimization_barrier(jnp.mean(retained * retained, axis=-1, keepdims=True)) + epsilon)
    gate_wide = gate_rows.astype(jnp.float32).reshape(SEQUENCE_LENGTH, RETENTION_HEADS, DV)
    gated = (jax.nn.silu(gate_wide) * scaled).astype(jnp.bfloat16).reshape(SEQUENCE_LENGTH, RETENTION_HEADS * DV)
    mixer_out = blocked_product(gated, out_weight, N_TP).astype(jnp.bfloat16)
    widened = channel_input.astype(jnp.float32)
    normed = (widened * lax.rsqrt(lax.optimization_barrier(jnp.mean(widened * widened, axis=-1, keepdims=True)) + epsilon) * norm_gain).astype(jnp.bfloat16)
    shared_result = blocked_product(swiglu_hidden(normed, shared_gate, shared_up), shared_down, N_TP)
    flat_expert = routes.reshape(-1)
    assign_count = flat_expert.shape[0]
    flat_token = jnp.arange(assign_count, dtype=jnp.int32) // TOPK
    flat_weight = route_weight.reshape(-1)
    limit = N_EP * N_TP * CAP

    def add_expert(total, expert):
        chosen = jnp.nonzero(flat_expert == expert, size=limit, fill_value=assign_count)[0].astype(jnp.int32)
        valid = chosen < assign_count
        safe = jnp.minimum(chosen, assign_count - 1)
        token_index = flat_token[safe]
        weight = jnp.where(valid, flat_weight[safe], 0.0)
        hidden = swiglu_hidden(normed[token_index], expert_gate[expert], expert_up[expert])
        result = blocked_product(hidden, expert_down[expert], N_TP).astype(jnp.bfloat16)
        result = lax.optimization_barrier(result)
        return (total.at[token_index].add(weight[:, None] * result.astype(jnp.float32)), None)
    routed, _ = lax.scan(add_expert, jnp.zeros((TOKENS_M, D), jnp.float32), jnp.arange(EXPERTS, dtype=jnp.int32))
    channel_out = (shared_result + routed).astype(jnp.bfloat16)
    return (mixer_out, channel_out)
```

```python
import functools

import jax
import jax.numpy as jnp
from jax import lax
from jax.experimental import pallas as pl
from jax.experimental.pallas import tpu as pltpu
from jax.sharding import PartitionSpec as P

BLOCK = 128
CORES = 2

epsilon = 1e-06
turn_base = 10000.0


def line_pairs(count, step, senders):
    return [
        (z * CORES + c, (z + step) * CORES + c)
        for z in range(count)
        for c in range(CORES)
        if senders(z) and 0 <= z + step < count
    ]


def line_gather(tree, count):
    move = lambda t, pairs: jax.tree.map(lambda a: lax.ppermute(a, "tp", pairs), t)
    from_left, from_right = [tree], [tree]
    for r in range(1, count):
        from_left.append(move(from_left[-1], line_pairs(count, 1, lambda z: z >= r - 1)))
        from_right.append(
            move(from_right[-1], line_pairs(count, -1, lambda z: z <= count - r))
        )
    blocks = [tree] + [
        jax.tree.map(lambda a, b: a + b, from_left[r], from_right[count - r])
        for r in range(1, count)
    ]
    return jax.tree.map(lambda *parts: jnp.stack(parts), *blocks)


def line_scatter(part, count):
    right = left = None
    for r in range(1, count):
        send_right, send_left = part(r), part(count - r)
        if right is not None:
            send_right = (send_right.astype(jnp.float32) + right.astype(jnp.float32)).astype(
                jnp.bfloat16
            )
            send_left = (send_left.astype(jnp.float32) + left.astype(jnp.float32)).astype(
                jnp.bfloat16
            )
        right = lax.ppermute(send_right, "tp", line_pairs(count, 1, lambda z: z <= r - 1))
        left = lax.ppermute(
            send_left, "tp", line_pairs(count, -1, lambda z: z >= count - r)
        )
    return part(0).astype(jnp.float32) + right.astype(jnp.float32) + left.astype(jnp.float32)


def swap_cores(array, tp_count):
    return lax.ppermute(array, "tp", [(i, i ^ 1) for i in range(tp_count)])


def swap_ep(array, k, ep_count):
    return lax.ppermute(array, "ep", [(i, i ^ k) for i in range(ep_count)])


def turned(rows, cosine, sine):
    wide = rows.astype(jnp.float32)
    return (wide * cosine + pltpu.roll(wide, wide.shape[1] // 2, 1) * sine).astype(jnp.bfloat16)


def state_kernel(key_ref, value_ref, cosine_ref, sine_ref, fade_ref, state_ref):
    heads, key_width, value_width = state_ref.shape
    for h in range(heads):
        keys = turned(
            key_ref[:, h * key_width : (h + 1) * key_width], cosine_ref[...], sine_ref[...]
        )
        faded = (keys.astype(jnp.float32) * fade_ref[:, h : h + 1]).astype(jnp.bfloat16)
        state_ref[h] = lax.dot_general(
            faded,
            value_ref[:, h * value_width : (h + 1) * value_width],
            (((0,), (0,)), ((), ())),
            preferred_element_type=jnp.float32,
        ).astype(state_ref.dtype)


def retention_kernel(
    query_ref, key_ref, value_ref, gate_ref, cosine_ref, sine_ref, column_ref, row_ref,
    entry_ref, out_ref, state,
):
    heads, key_width, value_width = state.shape

    @pl.when(pl.program_id(0) == 0)
    def _():
        state[...] = entry_ref[...]

    cosine, sine = cosine_ref[...], sine_ref[...]
    lower = lax.broadcasted_iota(jnp.int32, (BLOCK, BLOCK), 0) >= lax.broadcasted_iota(
        jnp.int32, (BLOCK, BLOCK), 1
    )
    for h in range(heads):
        key_cut = slice(h * key_width, (h + 1) * key_width)
        value_cut = slice(h * value_width, (h + 1) * value_width)
        queries = turned(query_ref[:, key_cut], cosine, sine)
        keys = turned(key_ref[:, key_cut], cosine, sine)
        values = value_ref[:, value_cut]
        column = column_ref[:, h : h + 1]
        row = row_ref[0, h : h + 1, :]
        end = column_ref[BLOCK - 1 : BLOCK, h : h + 1]
        scores = lax.dot_general(
            queries, keys, (((1,), (1,)), ((), ())), preferred_element_type=jnp.float32
        )
        spread = jnp.exp(jnp.where(lower, column - row, 0.0))
        weights = jnp.where(lower, scores * spread, 0.0).astype(jnp.bfloat16)
        before = state[h]
        retained = jnp.dot(weights, values, preferred_element_type=jnp.float32)
        retained = retained + jnp.exp(column) * jnp.dot(
            queries, before.astype(jnp.bfloat16), preferred_element_type=jnp.float32
        )
        faded = (keys.astype(jnp.float32) * jnp.exp(end - column)).astype(jnp.bfloat16)
        state[h] = jnp.exp(end) * before + lax.dot_general(
            faded, values, (((0,), (0,)), ((), ())), preferred_element_type=jnp.float32
        )
        scale = lax.rsqrt(jnp.mean(retained * retained, axis=1, keepdims=True) + epsilon)
        gate = gate_ref[:, value_cut].astype(jnp.float32)
        out_ref[:, value_cut] = (gate / (1.0 + jnp.exp(-gate)) * (retained * scale)).astype(
            jnp.bfloat16
        )


def retention(query_rows, key_rows, value_rows, gate_rows, log_decay):
    tokens = query_rows.shape[0]
    heads = log_decay.shape[0]
    key_width = query_rows.shape[1] // heads
    value_width = value_rows.shape[1] // heads
    blocks = tokens // BLOCK
    ep_count, ep_index = lax.axis_size("ep"), lax.axis_index("ep")
    half = key_width // 2
    position = (ep_index * tokens + jnp.arange(tokens, dtype=jnp.int32)).astype(jnp.float32)
    inverse = turn_base ** (-jnp.arange(half, dtype=jnp.float32) / half)
    angles = position[:, None] * inverse[None, :]
    cosine, sine = jnp.cos(angles), jnp.sin(angles)
    cosine = jnp.concatenate([cosine, cosine], axis=1)
    sine = jnp.concatenate([-sine, sine], axis=1)
    running = jnp.cumsum(log_decay.reshape(heads, blocks, BLOCK), axis=2)
    ends = running[:, :, -1]
    later = jnp.sum(ends, axis=1, keepdims=True) - jnp.cumsum(ends, axis=1)
    later = jnp.minimum(later, 0.0)
    fade = jnp.exp(ends[:, :, None] - running + later[:, :, None]).reshape(heads, tokens).T
    total = jnp.sum(ends, axis=1)
    vmem = pl.BlockSpec(memory_space=pltpu.VMEM)
    own_state = pl.pallas_call(
        state_kernel,
        out_shape=jax.ShapeDtypeStruct((heads, key_width, value_width), jnp.bfloat16),
        in_specs=[vmem] * 5,
        out_specs=vmem,
        cost_estimate=pl.CostEstimate(
            flops=2 * tokens * heads * key_width * value_width * 4,
            bytes_accessed=8 << 20,
            transcendentals=0,
        ),
    )(key_rows, value_rows, cosine, sine, fade)
    totals_sent = jnp.broadcast_to(total[:, None], (heads, 128))
    states, totals = [], [total]
    for k in range(1, ep_count):
        states.append(swap_ep(own_state, k, ep_count))
        totals.append(swap_ep(totals_sent, k, ep_count)[:, 0])
    entry = jnp.zeros((heads, key_width, value_width), jnp.float32)
    for k in range(1, ep_count):
        source = ep_index ^ k
        passed = jnp.zeros_like(total)
        for m in range(1, ep_count):
            between = ((ep_index ^ m) > source) & ((ep_index ^ m) < ep_index)
            passed = passed + jnp.where(between, totals[m], 0.0)
        share = jnp.where(source < ep_index, jnp.exp(passed), 0.0)
        entry = entry + share[:, None, None] * states[k - 1].astype(jnp.float32)
    columns = running.reshape(heads, tokens).T
    rows = running.transpose(1, 0, 2)
    by_block = lambda width: pl.BlockSpec((BLOCK, width), lambda n: (n, 0))
    whole = pl.BlockSpec((heads, key_width, value_width), lambda n: (0, 0, 0))
    return pl.pallas_call(
        retention_kernel,
        out_shape=jax.ShapeDtypeStruct((tokens, heads * value_width), jnp.bfloat16),
        grid=(blocks,),
        in_specs=[
            by_block(heads * key_width),
            by_block(heads * key_width),
            by_block(heads * value_width),
            by_block(heads * value_width),
            by_block(key_width),
            by_block(key_width),
            by_block(heads),
            pl.BlockSpec((1, heads, BLOCK), lambda n: (n, 0, 0)),
            whole,
        ],
        out_specs=by_block(heads * value_width),
        scratch_shapes=[pltpu.VMEM((heads, key_width, value_width), jnp.float32)],
        cost_estimate=pl.CostEstimate(
            flops=8 << 30, bytes_accessed=24 << 20, transcendentals=0
        ),
    )(query_rows, key_rows, value_rows, gate_rows, cosine, sine, columns, rows, entry)


def gated_pair(gate_part, up_part):
    return (jax.nn.silu(gate_part) * up_part).astype(jnp.bfloat16)


def summed(a, b):
    return (a.astype(jnp.float32) + b.astype(jnp.float32)).astype(jnp.bfloat16)


def local(
    query_rows, key_rows, value_rows, gate_rows, log_decay, out_weight, channel_input, norm_gain,
    routes, route_weight, expert_gate, expert_up, expert_down, shared_gate, shared_up, shared_down,
):
    ep_count, tp_count = lax.axis_size("ep"), lax.axis_size("tp")
    ep_index, tp_index = lax.axis_index("ep"), lax.axis_index("tp")
    chips = tp_count // CORES
    chip, core = tp_index // CORES, tp_index % CORES
    tokens_here, width = channel_input.shape
    topk = routes.shape[1]
    local_experts = expert_gate.shape[0]
    experts_all = ep_count * local_experts
    capacity = tokens_here * topk // experts_all + max(
        2, tokens_here * topk // (3 * experts_all)
    )

    wide = channel_input.astype(jnp.float32)
    normed = (
        wide * lax.rsqrt(jnp.mean(wide * wide, axis=-1, keepdims=True) + epsilon) * norm_gain
    ).astype(jnp.bfloat16)
    flat = routes.reshape(-1)
    onehot = (flat[:, None] == jnp.arange(experts_all, dtype=jnp.int32)[None, :]).astype(
        jnp.float32
    )
    count = tokens_here * topk
    before = (jnp.arange(count)[:, None] > jnp.arange(count)[None, :]).astype(jnp.float32)
    rank = jnp.sum(jnp.dot(before, onehot) * onehot, axis=1)
    notes = jnp.concatenate(
        [routes.astype(jnp.float32), rank.reshape(tokens_here, topk), route_weight], axis=1
    )
    notes = jnp.pad(notes, ((0, 0), (0, 128 - 3 * topk)))
    own_rows, notes_all = line_gather((normed, notes), chips)
    route_all = notes_all[:, :, :topk].astype(jnp.int32)
    rank_all = notes_all[:, :, topk : 2 * topk].astype(jnp.int32)
    weight_all = notes_all[:, :, 2 * topk : 3 * topk]
    place = jnp.arange(chips, dtype=jnp.int32)[:, None, None]
    turn = (route_all // local_experts) ^ ep_index
    slot = ((turn * local_experts + route_all % local_experts) * chips + place) * capacity
    slot = (slot + rank_all).reshape(chips * tokens_here, topk)
    slot_count = experts_all * chips * capacity
    slot_ids = jnp.arange(slot_count, dtype=jnp.int32)
    placing = sum(
        (slot_ids[:, None] == slot[None, :, t]).astype(jnp.bfloat16) for t in range(topk)
    )
    own_flat = own_rows.reshape(chips * tokens_here, width)
    outgoing = jnp.dot(placing, own_flat, preferred_element_type=jnp.float32).astype(jnp.bfloat16)
    outgoing = outgoing.reshape(ep_count, local_experts, chips * capacity, width)
    arrived = [outgoing[0]] + [swap_ep(outgoing[k], k, ep_count) for k in range(1, ep_count)]
    arrived_twin = [swap_cores(block, tp_count) for block in arrived]
    own_twin = swap_cores(own_flat, tp_count)

    gated = retention(query_rows, key_rows, value_rows, gate_rows, log_decay)
    mixer_count = query_rows.shape[0] // tp_count
    gated_parts = gated.reshape(chips, CORES, mixer_count, gated.shape[1])

    def mixer_for(which):
        mine = lax.dynamic_index_in_dim(gated_parts, which, 1, keepdims=False)
        product = jnp.dot(
            mine.reshape(chips * mixer_count, -1), out_weight, preferred_element_type=jnp.float32
        )
        return product.astype(jnp.bfloat16)

    mixer_half = summed(mixer_for(core), swap_cores(mixer_for(1 - core), tp_count))
    mixer_half = mixer_half.reshape(chips, mixer_count, width)
    mixer_out = line_scatter(
        lambda r: lax.dynamic_index_in_dim(mixer_half, (chip + chips - r) % chips, 0, False), chips
    ).astype(jnp.bfloat16)

    def experts_on(blocks, rows):
        routed = jnp.concatenate(blocks, axis=1)
        gate_part = jnp.einsum("emd,edf->emf", routed, expert_gate, preferred_element_type=jnp.float32)
        up_part = jnp.einsum("emd,edf->emf", routed, expert_up, preferred_element_type=jnp.float32)
        hidden = gated_pair(gate_part, up_part)
        routed_term = jnp.einsum(
            "emf,efd->emd", hidden, expert_down, preferred_element_type=jnp.float32
        ).astype(jnp.bfloat16)
        shared_hidden = gated_pair(
            jnp.dot(rows, shared_gate, preferred_element_type=jnp.float32),
            jnp.dot(rows, shared_up, preferred_element_type=jnp.float32),
        )
        shared_term = jnp.dot(
            shared_hidden, shared_down, preferred_element_type=jnp.float32
        ).astype(jnp.bfloat16)
        return routed_term, shared_term

    routed_twin, shared_twin = experts_on(arrived_twin, own_twin)
    routed_mine, shared_mine = experts_on(arrived, own_flat)
    routed = summed(routed_mine, swap_cores(routed_twin, tp_count))
    shared = summed(shared_mine, swap_cores(shared_twin, tp_count))
    routed = routed.reshape(local_experts, ep_count, chips * capacity, width)
    returned = [routed[:, 0]] + [swap_ep(routed[:, k], k, ep_count) for k in range(1, ep_count)]
    returned = jnp.stack(returned).reshape(slot_count, width)
    flat_weight = weight_all.reshape(chips * tokens_here, topk)
    mixing = sum(
        jnp.where(slot_ids[None, :] == slot[:, t : t + 1], flat_weight[:, t : t + 1], 0.0)
        for t in range(topk)
    )
    coarse = lax.reduce_precision(mixing, 8, 7)
    fine = (mixing - coarse).astype(jnp.bfloat16)
    coarse = coarse.astype(jnp.bfloat16)
    channel = (
        jnp.dot(coarse, returned, preferred_element_type=jnp.float32)
        + jnp.dot(fine, returned, preferred_element_type=jnp.float32)
        + shared.astype(jnp.float32)
    ).astype(jnp.bfloat16)
    channel = channel.reshape(chips, tokens_here, width)
    channel_out = line_scatter(lambda r: channel[r], chips).astype(jnp.bfloat16)
    return (mixer_out, channel_out)


def solution(mesh):
    in_specs = (
        P("ep", "tp"),
        P("ep", "tp"),
        P("ep", "tp"),
        P("ep", "tp"),
        P("tp", "ep"),
        P("tp", None),
        P(("ep", "tp"), None),
        P(),
        P(("ep", "tp"), None),
        P(("ep", "tp"), None),
        P("ep", None, "tp"),
        P("ep", None, "tp"),
        P("ep", "tp", None),
        P(None, "tp"),
        P(None, "tp"),
        P("tp", None),
    )
    out_specs = (P(("ep", "tp"), None), P(("ep", "tp"), None))
    return jax.shard_map(local, mesh=mesh, in_specs=in_specs, out_specs=out_specs, check_vma=False)
```

```python
import functools

import jax
import jax.numpy as jnp
from jax import lax
from jax.experimental import pallas as pl
from jax.experimental.pallas import tpu as pltpu
from jax.sharding import PartitionSpec as P

BLOCK = 128
CORES = 2

epsilon = 1e-06
turn_base = 10000.0


def shift_chips(array, r, count):
    pairs = [
        (z * CORES + c, (z + r) % count * CORES + c) for z in range(count) for c in range(CORES)
    ]
    return lax.ppermute(array, "tp", pairs)


def line_gather(array, count):
    return jnp.stack([array] + [shift_chips(array, r, count) for r in range(1, count)])


def line_scatter(part, count):
    total = part(0).astype(jnp.float32)
    for r in range(1, count):
        total = total + shift_chips(part(r), r, count).astype(jnp.float32)
    return total


def swap_cores(array, tp_count):
    return lax.ppermute(array, "tp", [(i, i ^ 1) for i in range(tp_count)])


def swap_ep(array, k, ep_count):
    return lax.ppermute(array, "ep", [(i, i ^ k) for i in range(ep_count)])


def turned(rows, cosine, sine):
    wide = rows.astype(jnp.float32)
    return (wide * cosine + pltpu.roll(wide, wide.shape[1] // 2, 1) * sine).astype(jnp.bfloat16)


def state_kernel(key_ref, value_ref, cosine_ref, sine_ref, fade_ref, state_ref):
    heads, key_width, value_width = state_ref.shape
    for h in range(heads):
        keys = turned(
            key_ref[:, h * key_width : (h + 1) * key_width], cosine_ref[...], sine_ref[...]
        )
        faded = (keys.astype(jnp.float32) * fade_ref[:, h : h + 1]).astype(jnp.bfloat16)
        state_ref[h] = lax.dot_general(
            faded,
            value_ref[:, h * value_width : (h + 1) * value_width],
            (((0,), (0,)), ((), ())),
            preferred_element_type=jnp.float32,
        ).astype(state_ref.dtype)


def retention_kernel(
    query_ref, key_ref, value_ref, gate_ref, cosine_ref, sine_ref, column_ref, row_ref,
    entry_ref, out_ref, state,
):
    heads, key_width, value_width = state.shape

    @pl.when(pl.program_id(0) == 0)
    def _():
        state[...] = entry_ref[...]

    cosine, sine = cosine_ref[...], sine_ref[...]
    lower = lax.broadcasted_iota(jnp.int32, (BLOCK, BLOCK), 0) >= lax.broadcasted_iota(
        jnp.int32, (BLOCK, BLOCK), 1
    )
    for h in range(heads):
        key_cut = slice(h * key_width, (h + 1) * key_width)
        value_cut = slice(h * value_width, (h + 1) * value_width)
        queries = turned(query_ref[:, key_cut], cosine, sine)
        keys = turned(key_ref[:, key_cut], cosine, sine)
        values = value_ref[:, value_cut]
        column = column_ref[:, h : h + 1]
        row = row_ref[0, h : h + 1, :]
        end = column_ref[BLOCK - 1 : BLOCK, h : h + 1]
        scores = lax.dot_general(
            queries, keys, (((1,), (1,)), ((), ())), preferred_element_type=jnp.float32
        )
        spread = jnp.exp(jnp.where(lower, column - row, 0.0))
        weights = jnp.where(lower, scores * spread, 0.0).astype(jnp.bfloat16)
        before = state[h]
        retained = jnp.dot(weights, values, preferred_element_type=jnp.float32)
        retained = retained + jnp.exp(column) * jnp.dot(
            queries, before.astype(jnp.bfloat16), preferred_element_type=jnp.float32
        )
        faded = (keys.astype(jnp.float32) * jnp.exp(end - column)).astype(jnp.bfloat16)
        state[h] = jnp.exp(end) * before + lax.dot_general(
            faded, values, (((0,), (0,)), ((), ())), preferred_element_type=jnp.float32
        )
        scale = lax.rsqrt(jnp.mean(retained * retained, axis=1, keepdims=True) + epsilon)
        gate = gate_ref[:, value_cut].astype(jnp.float32)
        out_ref[:, value_cut] = (gate / (1.0 + jnp.exp(-gate)) * (retained * scale)).astype(
            jnp.bfloat16
        )


def retention(query_rows, key_rows, value_rows, gate_rows, log_decay):
    tokens = query_rows.shape[0]
    heads = log_decay.shape[0]
    key_width = query_rows.shape[1] // heads
    value_width = value_rows.shape[1] // heads
    blocks = tokens // BLOCK
    ep_count, ep_index = lax.axis_size("ep"), lax.axis_index("ep")
    half = key_width // 2
    position = (ep_index * tokens + jnp.arange(tokens, dtype=jnp.int32)).astype(jnp.float32)
    inverse = turn_base ** (-jnp.arange(half, dtype=jnp.float32) / half)
    angles = position[:, None] * inverse[None, :]
    cosine, sine = jnp.cos(angles), jnp.sin(angles)
    cosine = jnp.concatenate([cosine, cosine], axis=1)
    sine = jnp.concatenate([-sine, sine], axis=1)
    running = jnp.cumsum(log_decay.reshape(heads, blocks, BLOCK), axis=2)
    ends = running[:, :, -1]
    later = jnp.sum(ends, axis=1, keepdims=True) - jnp.cumsum(ends, axis=1)
    later = jnp.minimum(later, 0.0)
    fade = jnp.exp(ends[:, :, None] - running + later[:, :, None]).reshape(heads, tokens).T
    total = jnp.sum(ends, axis=1)
    vmem = pl.BlockSpec(memory_space=pltpu.VMEM)
    own_state = pl.pallas_call(
        state_kernel,
        out_shape=jax.ShapeDtypeStruct((heads, key_width, value_width), jnp.bfloat16),
        in_specs=[vmem] * 5,
        out_specs=vmem,
        cost_estimate=pl.CostEstimate(
            flops=2 * tokens * heads * key_width * value_width * 4,
            bytes_accessed=8 << 20,
            transcendentals=0,
        ),
    )(key_rows, value_rows, cosine, sine, fade)
    totals_sent = jnp.broadcast_to(total[:, None], (heads, 128))
    states, totals = [], [total]
    for k in range(1, ep_count):
        states.append(swap_ep(own_state, k, ep_count))
        totals.append(swap_ep(totals_sent, k, ep_count)[:, 0])
    entry = jnp.zeros((heads, key_width, value_width), jnp.float32)
    for k in range(1, ep_count):
        source = ep_index ^ k
        passed = jnp.zeros_like(total)
        for m in range(1, ep_count):
            between = ((ep_index ^ m) > source) & ((ep_index ^ m) < ep_index)
            passed = passed + jnp.where(between, totals[m], 0.0)
        share = jnp.where(source < ep_index, jnp.exp(passed), 0.0)
        entry = entry + share[:, None, None] * states[k - 1].astype(jnp.float32)
    columns = running.reshape(heads, tokens).T
    rows = running.transpose(1, 0, 2)
    by_block = lambda width: pl.BlockSpec((BLOCK, width), lambda n: (n, 0))
    whole = pl.BlockSpec((heads, key_width, value_width), lambda n: (0, 0, 0))
    return pl.pallas_call(
        retention_kernel,
        out_shape=jax.ShapeDtypeStruct((tokens, heads * value_width), jnp.bfloat16),
        grid=(blocks,),
        in_specs=[
            by_block(heads * key_width),
            by_block(heads * key_width),
            by_block(heads * value_width),
            by_block(heads * value_width),
            by_block(key_width),
            by_block(key_width),
            by_block(heads),
            pl.BlockSpec((1, heads, BLOCK), lambda n: (n, 0, 0)),
            whole,
        ],
        out_specs=by_block(heads * value_width),
        scratch_shapes=[pltpu.VMEM((heads, key_width, value_width), jnp.float32)],
        cost_estimate=pl.CostEstimate(
            flops=8 << 30, bytes_accessed=24 << 20, transcendentals=0
        ),
    )(query_rows, key_rows, value_rows, gate_rows, cosine, sine, columns, rows, entry)


def gated_pair(gate_part, up_part):
    return (jax.nn.silu(gate_part) * up_part).astype(jnp.bfloat16)


def summed(a, b):
    return (a.astype(jnp.float32) + b.astype(jnp.float32)).astype(jnp.bfloat16)


def local(
    query_rows, key_rows, value_rows, gate_rows, log_decay, out_weight, channel_input, norm_gain,
    routes, route_weight, expert_gate, expert_up, expert_down, shared_gate, shared_up, shared_down,
):
    ep_count, tp_count = lax.axis_size("ep"), lax.axis_size("tp")
    ep_index, tp_index = lax.axis_index("ep"), lax.axis_index("tp")
    chips = tp_count // CORES
    chip, core = tp_index // CORES, tp_index % CORES
    tokens_here, width = channel_input.shape
    topk = routes.shape[1]
    local_experts = expert_gate.shape[0]
    experts_all = ep_count * local_experts
    capacity = tokens_here * topk // experts_all + max(
        2, tokens_here * topk // (3 * experts_all)
    )

    wide = channel_input.astype(jnp.float32)
    normed = (
        wide * lax.rsqrt(jnp.mean(wide * wide, axis=-1, keepdims=True) + epsilon) * norm_gain
    ).astype(jnp.bfloat16)
    flat = routes.reshape(-1)
    onehot = (flat[:, None] == jnp.arange(experts_all, dtype=jnp.int32)[None, :]).astype(
        jnp.float32
    )
    count = tokens_here * topk
    before = (jnp.arange(count)[:, None] > jnp.arange(count)[None, :]).astype(jnp.float32)
    rank = jnp.sum(jnp.dot(before, onehot) * onehot, axis=1)
    notes = jnp.concatenate(
        [routes.astype(jnp.float32), rank.reshape(tokens_here, topk), route_weight], axis=1
    )
    notes = jnp.pad(notes, ((0, 0), (0, 128 - 3 * topk)))
    own_rows = line_gather(normed, chips)
    notes_all = line_gather(notes, chips)
    log_decay, normed, notes = lax.optimization_barrier((log_decay, normed, notes))
    route_all = notes_all[:, :, :topk].astype(jnp.int32)
    rank_all = notes_all[:, :, topk : 2 * topk].astype(jnp.int32)
    weight_all = notes_all[:, :, 2 * topk : 3 * topk]
    place = jnp.arange(chips, dtype=jnp.int32)[:, None, None]
    turn = (route_all // local_experts) ^ ep_index
    slot = ((turn * local_experts + route_all % local_experts) * chips + place) * capacity
    slot = (slot + rank_all).reshape(chips * tokens_here, topk)
    slot_count = experts_all * chips * capacity
    slot_ids = jnp.arange(slot_count, dtype=jnp.int32)
    placing = sum(
        (slot_ids[:, None] == slot[None, :, t]).astype(jnp.bfloat16) for t in range(topk)
    )
    own_flat = own_rows.reshape(chips * tokens_here, width)
    outgoing = jnp.dot(placing, own_flat, preferred_element_type=jnp.float32).astype(jnp.bfloat16)
    outgoing = outgoing.reshape(ep_count, local_experts, chips * capacity, width)
    arrived = [outgoing[0]] + [swap_ep(outgoing[k], k, ep_count) for k in range(1, ep_count)]
    own_twin = swap_cores(own_flat, tp_count)

    gated = retention(query_rows, key_rows, value_rows, gate_rows, log_decay)
    mixer_count = query_rows.shape[0] // tp_count
    gated_parts = gated.reshape(chips, CORES, mixer_count, gated.shape[1])

    def mixer_for(which):
        mine = lax.dynamic_index_in_dim(gated_parts, which, 1, keepdims=False)
        product = jnp.dot(
            mine.reshape(chips * mixer_count, -1), out_weight, preferred_element_type=jnp.float32
        )
        return product.astype(jnp.bfloat16)

    mixer_twin, mixer_mine = mixer_for(1 - core), mixer_for(core)
    mixer_half = summed(mixer_mine, swap_cores(mixer_twin, tp_count))
    arrived, _ = lax.optimization_barrier((arrived, (mixer_twin, mixer_mine)))
    arrived_twin = [swap_cores(block, tp_count) for block in arrived]
    mixer_half = mixer_half.reshape(chips, mixer_count, width)
    mixer_out = line_scatter(
        lambda r: lax.dynamic_index_in_dim(mixer_half, (chip + r) % chips, 0, False), chips
    ).astype(jnp.bfloat16)

    def experts_on(blocks, rows):
        routed = jnp.concatenate(blocks, axis=1)
        gate_part = jnp.einsum("emd,edf->emf", routed, expert_gate, preferred_element_type=jnp.float32)
        up_part = jnp.einsum("emd,edf->emf", routed, expert_up, preferred_element_type=jnp.float32)
        hidden = gated_pair(gate_part, up_part)
        routed_term = jnp.einsum(
            "emf,efd->emd", hidden, expert_down, preferred_element_type=jnp.float32
        ).astype(jnp.bfloat16)
        shared_hidden = gated_pair(
            jnp.dot(rows, shared_gate, preferred_element_type=jnp.float32),
            jnp.dot(rows, shared_up, preferred_element_type=jnp.float32),
        )
        shared_term = jnp.dot(
            shared_hidden, shared_down, preferred_element_type=jnp.float32
        ).astype(jnp.bfloat16)
        return routed_term, shared_term

    routed_twin, shared_twin = experts_on(arrived_twin, own_twin)
    routed_mine, shared_mine = experts_on(arrived, own_flat)
    routed = summed(routed_mine, swap_cores(routed_twin, tp_count))
    shared = summed(shared_mine, swap_cores(shared_twin, tp_count))
    routed = routed.reshape(local_experts, ep_count, chips * capacity, width)
    returned = [routed[:, 0]] + [swap_ep(routed[:, k], k, ep_count) for k in range(1, ep_count)]
    returned = jnp.stack(returned).reshape(slot_count, width)
    flat_weight = weight_all.reshape(chips * tokens_here, topk)
    mixing = sum(
        jnp.where(slot_ids[None, :] == slot[:, t : t + 1], flat_weight[:, t : t + 1], 0.0)
        for t in range(topk)
    )
    coarse = lax.reduce_precision(mixing, 8, 7)
    fine = (mixing - coarse).astype(jnp.bfloat16)
    coarse = coarse.astype(jnp.bfloat16)
    channel = (
        jnp.dot(coarse, returned, preferred_element_type=jnp.float32)
        + jnp.dot(fine, returned, preferred_element_type=jnp.float32)
        + shared.astype(jnp.float32)
    ).astype(jnp.bfloat16)
    channel = channel.reshape(chips, tokens_here, width)
    channel_out = line_scatter(lambda r: channel[(chips - r) % chips], chips).astype(jnp.bfloat16)
    return (mixer_out, channel_out)


def solution(mesh):
    in_specs = (
        P("ep", "tp"),
        P("ep", "tp"),
        P("ep", "tp"),
        P("ep", "tp"),
        P("tp", "ep"),
        P("tp", None),
        P(("ep", "tp"), None),
        P(),
        P(("ep", "tp"), None),
        P(("ep", "tp"), None),
        P("ep", None, "tp"),
        P("ep", None, "tp"),
        P("ep", "tp", None),
        P(None, "tp"),
        P(None, "tp"),
        P("tp", None),
    )
    out_specs = (P(("ep", "tp"), None), P(("ep", "tp"), None))
    return jax.shard_map(local, mesh=mesh, in_specs=in_specs, out_specs=out_specs, check_vma=False)
```
